32 devices in a mesh: sp: 16 (over z, y, x), tp: 2 (over core).
Axes of the slice: x: 2, y: 2, z: 4, core: 2. Of those that a mesh axis runs over, the one named last changes fastest.
Arguments:
- queries: bfloat16 [4096, 1024], P('sp', 'tp'), may hold values from -6 to 6
- key_vectors: bfloat16 [4096, 1024], P('sp', 'tp'), may hold values from -6 to 6
- value_vectors: bfloat16 [4096, 1024], P('sp', 'tp'), may hold values from -6 to 6
- gate_inputs: bfloat16 [4096, 1024], P('sp', 'tp'), may hold values from -6 to 6
- log_decay: float32 [4096, 16], P('sp', 'tp'), may hold values from -1 to 0
- head_gain: float32 [1024], P('tp'), may hold values from 0.1 to 1.9
- out_weight: bfloat16 [1024, 2048], P('tp'), may hold values from -0.1875 to 0.1875
- residual: bfloat16 [4096, 2048], P(('sp', 'tp')), may hold values from -6 to 6
- norm_gain: float32 [2048], replicated, may hold values from 0.1 to 1.9
- expert_ids: int32 [4096, 2], P(('sp', 'tp')), may hold values from 0 to 15, all different within a row; in each aligned block of 128 rows (0 to 127, 128 to 255, ...) at most 32 rows name the same one
- expert_weights: float32 [4096, 2], P(('sp', 'tp')), may hold values from 0.2 to 1
- gate_experts: bfloat16 [16, 2048, 3584], P('sp', None, 'tp'), may hold values from -0.125 to 0.125
- up_experts: bfloat16 [16, 2048, 3584], P('sp', None, 'tp'), may hold values from -0.125 to 0.125
- down_experts: bfloat16 [16, 3584, 2048], P('sp', 'tp'), may hold values from -0.09375 to 0.09375
Outputs:
- layer_out: bfloat16 [4096, 2048], P(('sp', 'tp'))
The draws below stay inside these ranges and needn't reach their ends.
Inputs may be any that keep to these rules, and one draw needn't show every extreme that they name: `expert_ids`: the 2 experts of a token differ. No expert is named more than 32 times in the rows of one device, and in some device some expert is named exactly 32 times.
All inputs are finite; a program needn't handle non-finite values.
Results may differ from the reference program's by a relative error of at most 0.014.
Values may be sent and summed in bfloat16 or wider, within the bound.
No kernel may reach another device: no remote copies, remote signals or barrier semaphores. Data moves between devices by JAX's collectives and lax.ppermute only.
A program may use at most 128 MiB of HBM per device.

```python
import math
import jax
import jax.numpy as jnp
import numpy as np
from jax import lax

D = 2048
MEMORY_CHANNELS = 16
HD = 64
FF = 3584
TOP = 2
BLOCK = 128
TOK_DEV = 256
STRING_LENGTH = 4096
EXPERTS = 16
CAP = 32
N_SP = 16
N_TP = 2


def draw_log_decay(key, part):
    concurrent_lanes = jax.random.split(key, 7)
    fast_share = 0.5
    fast = jax.random.uniform(concurrent_lanes[0], (MEMORY_CHANNELS,), jnp.float32) < fast_share
    fast_rate = jax.random.uniform(concurrent_lanes[1], (MEMORY_CHANNELS,), jnp.float32, 1.0 / 100.0, 1.0 / 30.0)
    slow_rate = jax.random.uniform(concurrent_lanes[2], (MEMORY_CHANNELS,), jnp.float32, 0.2, 0.6) / STRING_LENGTH
    reference_shrink_speed = jnp.where(fast, fast_rate, slow_rate)
    shrink_multipliers = jnp.exp(jax.random.uniform(concurrent_lanes[3], (STRING_LENGTH // BLOCK, MEMORY_CHANNELS), jnp.float32, -0.7, 0.7))
    shrink_multipliers = jnp.repeat(shrink_multipliers, BLOCK, axis=0)
    stochastic_jitter = jax.random.uniform(concurrent_lanes[4], (STRING_LENGTH, MEMORY_CHANNELS), jnp.float32, 0.5, 1.5)
    spike_occurrences = jax.random.uniform(concurrent_lanes[5], (STRING_LENGTH, MEMORY_CHANNELS), jnp.float32) < 2.0 / STRING_LENGTH
    surviving_proportion = jax.random.uniform(concurrent_lanes[6], (STRING_LENGTH, MEMORY_CHANNELS), jnp.float32, 0.5, 0.8)
    closing_result = -reference_shrink_speed[None, :] * shrink_multipliers * stochastic_jitter + jnp.where(spike_occurrences, jnp.log(surviving_proportion), 0.0)
    return closing_result.astype(jnp.float32)


def steps_of(stream_key, dims, shards, smallest, largest):
    loudness = 1.0
    for position, shards_of in shards:
        draws = jax.random.uniform(jax.random.fold_in(jax.random.fold_in(stream_key, 6), position), (shards_of,), jnp.float32, smallest / len(shards), largest / len(shards))
        loudness = loudness * jnp.repeat(jnp.exp(draws), dims[position] // shards_of).reshape((-1,) + (1,) * (len(dims) - 1 - position))
    return loudness


def assign_block(rng, own, number, rows, count, top, most, lean):
    ranking = jax.random.permutation(rng, count)
    packed, usual = portions_of(count, rows * top, most, lean, True), portions_of(count, rows * top, most, lean, False)
    places = jnp.arange(count)

    def named(sizes, rotation):
        used = int((sizes > 0).sum())
        fixed = max(1, used // 4)
        moved = fixed + (places - fixed + rotation * (used - fixed)) % max(1, count - fixed)
        return jnp.zeros((count,), jnp.int32).at[ranking[jnp.where(places < fixed, places, moved)]].set(jnp.asarray(sizes, jnp.int32))

    sizes = jnp.where(number % 4 == 0, named(packed, number // 4), named(usual, number - number // 4 - 1))
    mixed = jax.random.permutation(jax.random.fold_in(own, 3), count)
    donor, receiver = mixed[0:count // 2 * 2:2], mixed[1:count // 2 * 2:2]
    slack = jnp.minimum(sizes[donor] - 1, most - sizes[receiver]) // 2
    slack = jnp.where((donor == ranking[0]) | (receiver == ranking[0]) | (sizes[receiver] == 0), 0, jnp.maximum(slack, 0))
    moved = jax.random.randint(jax.random.fold_in(own, 4), (count // 2,), 0, 1 << 20) % (slack + 1)
    sizes = sizes.at[donor].add(-moved).at[receiver].add(moved)
    items = jnp.searchsorted(jnp.cumsum(sizes), jnp.arange(rows * top), side="right").astype(jnp.int32)
    listing = items.reshape(top, rows).T
    listing = listing[jax.random.permutation(jax.random.fold_in(own, 1), rows)]
    rotation = jax.random.randint(jax.random.fold_in(own, 2), (rows, 1), 0, top)
    return jnp.take_along_axis(listing, (jnp.arange(top)[None, :] + rotation) % top, axis=1)


def portions_of(amount, total, limit, skew, full):
    weights = [(1 << 20) // math.isqrt(grade ** skew) + 1 for grade in range(1, amount + 1)]
    largest = limit if full else min(limit, max(-(-total // amount), total * weights[0] // sum(weights)))
    least = 1 if total - largest >= amount - 1 else 0
    counts, spare = [largest] + [least] * (amount - 1), total - largest - least * (amount - 1)
    while spare > 0:
        free = [i for i in range(1, amount) if counts[i] < largest] or [i for i in range(1, amount) if counts[i] < limit]
        pool, budget = sum([weights[i] for i in free]), spare
        for i in free:
            more = min(limit - counts[i], max(1, budget * weights[i] // pool), spare)
            counts[i] = counts[i] + more
            spare = spare - more
    return np.array(counts)


def normal_values(own_key, extent, width, reach, cuts=(), kind=jnp.bfloat16):
    values = width * jax.random.normal(own_key, extent, jnp.float32)
    if cuts:
        values = values * steps_of(own_key, extent, cuts, -0.22, 0.18)
    return jnp.clip(values, -reach, reach).astype(kind)


def setup_inputs(seed: int = 0) -> dict:
    streams_of = jax.random.split(jax.random.key(seed), 15)
    queries = normal_values(streams_of[0], (STRING_LENGTH, MEMORY_CHANNELS * HD), 1.0, 6.0, ((0, 16), (1, 2)))
    key_vectors = normal_values(streams_of[1], (STRING_LENGTH, MEMORY_CHANNELS * HD), 1.0, 6.0, ((0, 16), (1, 2)))
    value_vectors = normal_values(streams_of[2], (STRING_LENGTH, MEMORY_CHANNELS * HD), 1.0, 6.0, ((0, 16), (1, 2)))
    gate_inputs = normal_values(streams_of[3], (STRING_LENGTH, MEMORY_CHANNELS * HD), 1.0, 6.0, ((0, 16), (1, 2)))
    log_decay = draw_log_decay(jax.random.fold_in(streams_of[14], 71), 0)
    head_gain = jnp.clip(1.0 + 0.18 * jax.random.normal(streams_of[5], (MEMORY_CHANNELS * HD,), jnp.float32), 0.1, 1.9)
    out_weight = normal_values(streams_of[6], (MEMORY_CHANNELS * HD, D), (MEMORY_CHANNELS * HD) ** -0.5, 0.1875, ((0, 2),))
    residual = normal_values(streams_of[7], (STRING_LENGTH, D), 1.0, 6.0, ((0, 32),))
    norm_gain = jnp.clip(1.0 + 0.18 * jax.random.normal(streams_of[8], (D,), jnp.float32), 0.1, 1.9)
    expert_ids_keys = jax.random.split(jax.random.fold_in(streams_of[9], 1), STRING_LENGTH // (TOK_DEV // N_TP))
    expert_ids_turns = jax.random.permutation(jax.random.fold_in(streams_of[9], 3), STRING_LENGTH // (TOK_DEV // N_TP))
    expert_ids = jax.vmap(lambda own, number: assign_block(jax.random.fold_in(streams_of[9], 2), own, number, TOK_DEV // N_TP, EXPERTS, TOP, CAP, 1))(expert_ids_keys, expert_ids_turns).reshape((STRING_LENGTH, TOP))
    expert_weights = jnp.clip(0.2 + 0.8 * jax.random.uniform(streams_of[10], (STRING_LENGTH, TOP), jnp.float32) ** steps_of(streams_of[10], (STRING_LENGTH, TOP), ((0, 32),), -0.2, 0.2), 0.2, 1.0)
    gate_experts = normal_values(streams_of[11], (EXPERTS, D, FF), D ** -0.5, 0.125, ((0, 16), (2, 2)))
    up_experts = normal_values(streams_of[12], (EXPERTS, D, FF), D ** -0.5, 0.125, ((0, 16), (2, 2)))
    down_experts = normal_values(streams_of[13], (EXPERTS, FF, D), FF ** -0.5, 0.09375, ((0, 16), (1, 2)))
    return dict(queries=queries, key_vectors=key_vectors, value_vectors=value_vectors, gate_inputs=gate_inputs, log_decay=log_decay, head_gain=head_gain, out_weight=out_weight, residual=residual, norm_gain=norm_gain, expert_ids=expert_ids, expert_weights=expert_weights, gate_experts=gate_experts, up_experts=up_experts, down_experts=down_experts)


def rotate(block, places):
    half_size = block.shape[-1] // 2
    frequency = 10000.0 ** (-jnp.arange(half_size, dtype=jnp.float32) / half_size)
    angles = places.astype(jnp.float32)[:, None, None] * frequency
    first_half = block[..., :half_size]
    second = block[..., half_size:]
    return jnp.concatenate([first_half * jnp.cos(angles) - second * jnp.sin(angles), second * jnp.cos(angles) + first_half * jnp.sin(angles)], axis=-1)

def to_blocks(source, blocks):
    shaped = source.reshape((blocks, source.shape[0] // blocks) + source.shape[1:])
    return jnp.swapaxes(shaped, 1, 2)

def from_blocks(source):
    shaped = jnp.swapaxes(source, 1, 2)
    return shaped.reshape((shaped.shape[0] * shaped.shape[1],) + shaped.shape[2:])

def block_step(carried_state, inputs):
    query_rows, key_rows, value_rows, decay_rows = inputs
    cumulative = jnp.cumsum(decay_rows, axis=1)
    log_gaps = cumulative[:, :, None] - cumulative[:, None, :]
    offsets = jnp.arange(decay_rows.shape[1])
    causal = offsets[:, None] >= offsets[None, :]
    decay_weight = jnp.where(causal, jnp.exp(jnp.where(causal, log_gaps, 0.0)), 0.0)
    scores = jnp.einsum('htd,hsd->hts', query_rows, key_rows, precision=lax.Precision.HIGHEST) * decay_weight
    within = jnp.einsum('hts,hse->hte', scores, value_rows, precision=lax.Precision.HIGHEST)
    carried = jnp.einsum('htd,hde->hte', query_rows * jnp.exp(cumulative)[:, :, None], carried_state, precision=lax.Precision.HIGHEST)
    last_log = cumulative[:, -1:]
    fresh_state = jnp.einsum('hsd,hse->hde', key_rows * jnp.exp(last_log - cumulative)[:, :, None], value_rows, precision=lax.Precision.HIGHEST)
    return (jnp.exp(last_log)[:, :, None] * carried_state + fresh_state, within + carried)

def round_trip(array):
    return lax.optimization_barrier(array.astype(jnp.bfloat16)).astype(jnp.float32)

def reference(queries, key_vectors, value_vectors, gate_inputs, log_decay, head_gain, out_weight, residual, norm_gain, expert_ids, expert_weights, gate_experts, up_experts, down_experts):
    places = jnp.arange(STRING_LENGTH, dtype=jnp.int32)
    turned_queries = rotate(queries.astype(jnp.float32).reshape(STRING_LENGTH, MEMORY_CHANNELS, HD), places)
    turned_keys = rotate(key_vectors.astype(jnp.float32).reshape(STRING_LENGTH, MEMORY_CHANNELS, HD), places) * HD ** (-0.5)
    value_float = value_vectors.astype(jnp.float32).reshape(STRING_LENGTH, MEMORY_CHANNELS, HD)
    blocks = STRING_LENGTH // BLOCK
    inputs = (to_blocks(turned_queries, blocks), to_blocks(turned_keys, blocks), to_blocks(value_float, blocks), to_blocks(log_decay, blocks))
    _, pieces = lax.scan(block_step, jnp.zeros((MEMORY_CHANNELS, HD, HD), jnp.float32), inputs)
    retained = from_blocks(pieces)
    squares = lax.optimization_barrier(jnp.mean(retained * retained, axis=-1, keepdims=True))
    normed = retained * lax.rsqrt(squares + 1e-06) * head_gain.reshape(MEMORY_CHANNELS, HD)
    normed = (normed.reshape(STRING_LENGTH, MEMORY_CHANNELS * HD) * jax.nn.silu(gate_inputs.astype(jnp.float32))).astype(jnp.bfloat16)
    half_heads = MEMORY_CHANNELS * HD // N_TP
    projected = jnp.zeros((STRING_LENGTH, D), jnp.float32)
    for section in range(N_TP):
        partial_value = jnp.dot(normed[:, section * half_heads:(section + 1) * half_heads], out_weight[section * half_heads:(section + 1) * half_heads], preferred_element_type=jnp.float32)
        projected = projected + round_trip(partial_value)
    mixed_rows = (residual.astype(jnp.float32) + projected).astype(jnp.bfloat16)
    mixed_float = mixed_rows.astype(jnp.float32)
    normed_rows = (mixed_float * lax.rsqrt(lax.optimization_barrier(jnp.mean(mixed_float * mixed_float, axis=-1, keepdims=True)) + 1e-06) * norm_gain).astype(jnp.bfloat16)
    sources = N_SP * N_TP
    flat_routes = expert_ids.reshape(sources, -1)
    onehot = (flat_routes[:, :, None] == jnp.arange(EXPERTS, dtype=jnp.int32)[None, None, :]).astype(jnp.int32)
    slot_rank = lax.optimization_barrier(jnp.sum(jnp.cumsum(onehot, axis=1) * onehot, axis=2)) - 1
    slot_index = (jnp.arange(sources, dtype=jnp.int32)[:, None] * CAP + slot_rank).astype(jnp.int32)
    token_index = (jnp.arange(STRING_LENGTH * TOP, dtype=jnp.int32) // TOP).reshape(sources, -1)
    table = jnp.zeros((EXPERTS, sources * CAP), jnp.int32).at[flat_routes, slot_index].set(token_index)
    slot_weight = jnp.zeros((EXPERTS, sources * CAP), expert_weights.dtype).at[flat_routes, slot_index].set(expert_weights.reshape(sources, -1))
    half_ff = FF // N_TP

    def expert_step(total, inputs):
        gate_matrix, up_matrix, down_matrix, index_rows, weight_rows = inputs
        batch = normed_rows[index_rows].astype(jnp.float32)
        gate_value = jnp.dot(batch, gate_matrix.astype(jnp.float32), precision=lax.Precision.HIGHEST)
        up_value = jnp.dot(batch, up_matrix.astype(jnp.float32), precision=lax.Precision.HIGHEST)
        hidden = round_trip(jax.nn.silu(gate_value) * up_value)
        summed = jnp.zeros((batch.shape[0], D), jnp.float32)
        for section in range(N_TP):
            partial_value = jnp.dot(hidden[:, section * half_ff:(section + 1) * half_ff], down_matrix[section * half_ff:(section + 1) * half_ff].astype(jnp.float32), precision=lax.Precision.HIGHEST)
            summed = summed + round_trip(partial_value)
        expert_out = round_trip(summed)
        return (total.at[index_rows].add(weight_rows[:, None] * expert_out), None)
    expert_sum, _ = lax.scan(expert_step, jnp.zeros((STRING_LENGTH, D), jnp.float32), (gate_experts, up_experts, down_experts, table, slot_weight))
    return (mixed_rows.astype(jnp.float32) + expert_sum).astype(jnp.bfloat16)
```

```python
import functools

import jax
import jax.numpy as jnp
import numpy as np
from jax import lax
from jax.experimental import pallas as pl
from jax.experimental.pallas import tpu as pltpu
from jax.sharding import PartitionSpec as P

BF16 = jnp.bfloat16
F32 = jnp.float32
LANES = 128
NEG = -1e30


def dot(a, b, dims=((1,), (0,)), precision=None):
    return lax.dot_general(a, b, (dims, ((), ())), precision=precision, preferred_element_type=F32)


def params(vmem=48):
    return pltpu.CompilerParams(vmem_limit_bytes=vmem * 1024 * 1024)


def lane_iota(rows, lanes=LANES):
    return lax.broadcasted_iota(jnp.int32, (rows, lanes), 1)


def row_iota(rows, lanes=LANES):
    return lax.broadcasted_iota(jnp.int32, (rows, lanes), 0)


def angles(base_ref, cos_ref, sin_ref):
    cos_base, sin_base = base_ref[0:1, :], base_ref[1:2, :]
    cos_t, sin_t = cos_ref[...], sin_ref[...]
    return cos_base * cos_t - sin_base * sin_t, sin_base * cos_t + cos_base * sin_t


def turn(x, cos, sin, size):
    half = size // 2
    first = lane_iota(x.shape[0]) % size < half
    other = jnp.where(first, pltpu.roll(x, LANES - half, 1), pltpu.roll(x, half, 1))
    return x * cos + other * sin


def cumulative_of(decay_ref):
    rows = decay_ref.shape[0]
    lower = (row_iota(rows, rows) >= lane_iota(rows, rows)).astype(F32)
    return dot(lower, decay_ref[...], precision=lax.Precision.HIGHEST)


def spread(table, pair, rows, size):
    each = LANES // size
    out = table[:, pair * each : pair * each + 1]
    lane = lane_iota(rows)
    wide = jnp.broadcast_to(out, (rows, LANES))
    for i in range(1, each):
        wide = jnp.where(lane >= i * size, table[:, pair * each + i : pair * each + i + 1], wide)
    return wide


def state_kernel(k_ref, v_ref, decay_ref, base_ref, cos_ref, sin_ref, out_ref, *, size):
    rows, channels = k_ref.shape
    pairs = channels // LANES
    each = LANES // size
    cos, sin = angles(base_ref, cos_ref, sin_ref)
    cumulative = cumulative_of(decay_ref)
    total = cumulative[rows - 1 : rows, :]
    end = jnp.exp(total - cumulative)
    lane = lane_iota(size)
    for pair in range(pairs):
        cols = slice(pair * LANES, (pair + 1) * LANES)
        key = turn(k_ref[:, cols].astype(F32), cos, sin, size) * size ** (-0.5)
        key = (key * spread(end, pair, rows, size)).astype(BF16)
        full = dot(key, v_ref[:, cols], ((0,), (0,)))
        packed = full[0:size]
        for i in range(1, each):
            packed = jnp.where(lane >= i * size, full[i * size : (i + 1) * size], packed)
        out_ref[pair * size : (pair + 1) * size, :] = packed.astype(BF16)
    high = [spread(total, pair, 1, size) for pair in range(pairs)]
    low = [h - h.astype(BF16).astype(F32) for h in high]
    fill = [jnp.zeros((16 - 2 * pairs, LANES), F32)]
    out_ref[pairs * size : pairs * size + 16, :] = jnp.concatenate(high + low + fill, 0).astype(BF16)


def within_kernel(
    q_ref, k_ref, v_ref, decay_ref, base_ref, cos_ref, sin_ref, within_ref, scaled_ref, *, size
):
    rows, channels = k_ref.shape
    pairs = channels // LANES
    each = LANES // size
    cos, sin = angles(base_ref, cos_ref, sin_ref)
    cumulative = cumulative_of(decay_ref)
    upper = (row_iota(rows, rows) <= lane_iota(rows, rows)).astype(F32)
    across = dot(decay_ref[...], upper, ((0,), (0,)), precision=lax.Precision.HIGHEST)
    grown = jnp.exp(cumulative)
    causal = row_iota(rows, rows) >= lane_iota(rows, rows)
    lane = lane_iota(rows)
    for pair in range(pairs):
        cols = slice(pair * LANES, (pair + 1) * LANES)
        key = turn(k_ref[:, cols].astype(F32), cos, sin, size) * size ** (-0.5)
        query = turn(q_ref[:, cols].astype(F32), cos, sin, size)
        scaled_ref[:, cols] = (query * spread(grown, pair, rows, size)).astype(BF16)
        query = query.astype(BF16)
        value = v_ref[:, cols]
        result = jnp.zeros((rows, LANES), F32)
        for i in range(each):
            head = pair * each + i
            mine = (lane >= i * size) & (lane < (i + 1) * size)
            scores = dot(query, jnp.where(mine, key, 0.0).astype(BF16), ((1,), (1,)))
            gap = cumulative[:, head : head + 1] - across[head : head + 1, :]
            weight = jnp.exp(jnp.where(causal, gap, NEG))
            got = dot((scores * weight).astype(BF16), value)
            result = jnp.where(mine, got, result)
        within_ref[:, cols] = result


def normed_kernel(within_ref, scaled_ref, state_ref, gain_ref, gate_ref, out_ref, *, size):
    rows, channels = within_ref.shape
    each = LANES // size
    lane = lane_iota(rows)
    lane_s = lane_iota(size)
    for pair in range(channels // LANES):
        cols = slice(pair * LANES, (pair + 1) * LANES)
        packed = state_ref[pair * size : (pair + 1) * size, :]
        blocks = [
            jnp.where((lane_s >= i * size) & (lane_s < (i + 1) * size), packed, 0.0)
            for i in range(each)
        ]
        state = jnp.concatenate(blocks, 0).astype(BF16)
        retained = within_ref[:, cols] + dot(scaled_ref[:, cols], state)
        squares = retained * retained
        mean = jnp.zeros((rows, LANES), F32)
        for i in range(each):
            mine = (lane >= i * size) & (lane < (i + 1) * size)
            part = jnp.sum(jnp.where(mine, squares, 0.0), axis=1, keepdims=True) * (1.0 / size)
            mean = jnp.where(mine, part, mean)
        gate = gate_ref[:, cols].astype(F32)
        out = retained * lax.rsqrt(mean + 1e-06) * gain_ref[:, cols]
        out_ref[:, cols] = (out * (gate / (1.0 + jnp.exp(-gate)))).astype(BF16)


def split_state(packed, pairs, size):
    state = packed[: pairs * size].astype(F32).reshape(pairs, size, LANES)
    tail = packed[pairs * size :].astype(F32)
    return state, (tail[:pairs] + tail[pairs : 2 * pairs])[:, None, :]


def join_state(state, total, pairs, size):
    total = total[:, 0, :]
    high = total.astype(BF16)
    low = (total - high.astype(F32)).astype(BF16)
    fill = jnp.zeros((16 - 2 * pairs, LANES), BF16)
    return jnp.concatenate([state.astype(BF16).reshape(pairs * size, LANES), high, low, fill], 0)


def radices_of(count):
    out = []
    while count > 1:
        radix = next(r for r in (4, 2, 3, count) if count % r == 0)
        out.append(radix)
        count //= radix
    return out


def prefix_states(own, pairs, size):
    count = lax.axis_size("sp")
    place = lax.axis_index("sp")
    stride = 1
    before_s = jnp.zeros((pairs, size, LANES), F32)
    before_d = jnp.zeros((pairs, 1, LANES), F32)
    levels = radices_of(count)
    for level, radix in enumerate(levels):
        last = level == len(levels) - 1
        digit = (place // stride) % radix
        got = []
        for k in range(1, radix):
            pairs_of = []
            for j in range(count):
                d = (j // stride) % radix
                if last and d + k >= radix:
                    continue
                pairs_of.append((j, j + ((d + k) % radix - d) * stride))
            got.append(split_state(lax.ppermute(own, "sp", pairs_of), pairs, size))
        own_s, own_d = split_state(own, pairs, size)
        early_s = jnp.zeros_like(own_s)
        early_d = jnp.zeros_like(own_d)
        for k in range(1, radix):
            use = jnp.where(digit >= k, 1.0, 0.0)
            early_s = early_s + use * jnp.exp(early_d) * got[k - 1][0]
            early_d = early_d + use * got[k - 1][1]
        if not last:
            all_s = jnp.zeros_like(own_s)
            all_d = jnp.zeros_like(own_d)
            for k in range(1, radix):
                use = jnp.where(digit < k, 1.0, 0.0)
                all_s = all_s + use * jnp.exp(all_d) * got[k - 1][0]
                all_d = all_d + use * got[k - 1][1]
            all_s = all_s + jnp.exp(all_d) * own_s
            all_d = all_d + own_d
            all_s = all_s + jnp.exp(all_d) * early_s
            all_d = all_d + early_d
            own = join_state(all_s, all_d, pairs, size)
        before_s = before_s + jnp.exp(before_d) * early_s
        before_d = before_d + early_d
        stride *= radix
    return before_s.reshape(pairs * size, LANES)


def slots_of(ids, capacity, slots):
    tokens = ids.shape[0]
    lane = lane_iota(tokens).astype(F32)
    named = [lane == ids[:, j : j + 1] for j in range(ids.shape[1])]
    member = functools.reduce(jnp.logical_or, named).astype(BF16)
    strict = (row_iota(tokens, tokens) > lane_iota(tokens, tokens)).astype(BF16)
    rank = dot(strict, member)
    place = lane_iota(tokens, slots).astype(F32)
    out = []
    for j, hit in enumerate(named):
        slot = ids[:, j : j + 1] * capacity + jnp.sum(jnp.where(hit, rank, 0.0), 1, keepdims=True)
        out.append(place == slot)
    return out


def dispatch_kernel(
    a_ref, b_ref, wa_ref, wb_ref, res_ref, gain_ref, ids_ref, mixed_ref, out_ref, *, capacity
):
    projected = dot(a_ref[...], wa_ref[...]).astype(BF16).astype(F32)
    projected = projected + dot(b_ref[...], wb_ref[...]).astype(BF16).astype(F32)
    mixed = (res_ref[...].astype(F32) + projected).astype(BF16)
    mixed_ref[...] = mixed
    wide = mixed.astype(F32)
    scale = lax.rsqrt(jnp.mean(wide * wide, axis=1, keepdims=True) + 1e-06)
    rows = (wide * scale * gain_ref[...]).astype(BF16)
    hot = functools.reduce(jnp.logical_or, slots_of(ids_ref[...], capacity, out_ref.shape[0]))
    out_ref[...] = dot(hot.astype(BF16), rows, ((0,), (0,))).astype(BF16)


def expert_kernel(own_ref, oth_ref, gate_ref, up_ref, down_ref, pown_ref, poth_ref, acc_ref):
    step = pl.program_id(0)
    count = own_ref.shape[0]
    rows = jnp.concatenate([own_ref[...], oth_ref[...]], 0)
    gate = dot(rows, gate_ref[...])
    up = dot(rows, up_ref[...])
    hidden = (gate / (1.0 + jnp.exp(-gate)) * up).astype(BF16)
    part = dot(hidden, down_ref[...])

    @pl.when(step == 0)
    def _():
        acc_ref[...] = part

    @pl.when(step > 0)
    def _():
        acc_ref[...] += part

    @pl.when(step == pl.num_programs(0) - 1)
    def _():
        pown_ref[...] = acc_ref[:count].astype(BF16)
        poth_ref[...] = acc_ref[count:].astype(BF16)


def experts_call(own, oth, gate, up, down, name):
    rows, width = own.shape
    hidden = gate.shape[2]
    tile = next(t for t in (256, 128, hidden) if hidden % t == 0)
    whole = pl.BlockSpec((rows, width), lambda i: (0, 0))
    return pl.pallas_call(
        expert_kernel,
        grid=(hidden // tile,),
        in_specs=[
            whole,
            whole,
            pl.BlockSpec((None, width, tile), lambda i: (0, 0, i)),
            pl.BlockSpec((None, width, tile), lambda i: (0, 0, i)),
            pl.BlockSpec((None, tile, width), lambda i: (0, i, 0)),
        ],
        out_specs=[whole, whole],
        out_shape=[jax.ShapeDtypeStruct((rows, width), BF16)] * 2,
        scratch_shapes=[pltpu.VMEM((2 * rows, width), F32)],
        compiler_params=params(),
        cost_estimate=pl.CostEstimate(
            flops=2 * rows * 6 * width * hidden,
            bytes_accessed=6 * width * hidden,
            transcendentals=2 * rows * hidden,
        ),
        name=name,
    )(own, oth, gate, up, down)


def gather_sum(ret, ids, weights, capacity):
    hots = slots_of(ids, capacity, ret.shape[0])
    total = None
    for j, hot in enumerate(hots):
        part = dot(hot.astype(BF16), ret) * weights[:, j : j + 1]
        total = part if total is None else total + part
    return total


def back_kernel(ret_ref, ids_ref, weights_ref, out_ref, *, capacity):
    out_ref[...] = gather_sum(ret_ref[...], ids_ref[...], weights_ref[...], capacity).astype(BF16)


def final_kernel(mixed_ref, part_ref, far_ref, out_ref):
    total = part_ref[...] + far_ref[...].astype(F32)
    out_ref[...] = (mixed_ref[...].astype(F32) + total).astype(BF16)


def own_kernel(ret_ref, ids_ref, weights_ref, out_ref, *, capacity):
    out_ref[...] = gather_sum(ret_ref[...], ids_ref[...], weights_ref[...], capacity)


def call(kernel, outs, args, name, **static):
    out_shape = [jax.ShapeDtypeStruct(s, d) for s, d in outs]
    return pl.pallas_call(
        functools.partial(kernel, **static) if static else kernel,
        out_shape=out_shape,
        compiler_params=params(),
        name=name,
    )(*args)


def shards(
    queries,
    key_vectors,
    value_vectors,
    gate_inputs,
    log_decay,
    head_gain,
    out_weight,
    residual,
    norm_gain,
    expert_ids,
    expert_weights,
    gate_experts,
    up_experts,
    down_experts,
):
    tok_dev, channels = queries.shape
    heads = log_decay.shape[1]
    size = channels // heads
    pairs = channels // LANES
    tokens, width = residual.shape
    count = lax.axis_size("sp")
    cores = lax.axis_size("tp")
    half = count // 2
    capacity = 2 * tok_dev // count
    place = lax.axis_index("sp")
    core = lax.axis_index("tp")
    across = [(j, (j + half) % count) for j in range(count)]
    swap = [(c, cores - 1 - c) for c in range(cores)]
    groups = [list(range(half)), list(range(half, count))]

    far_res = lax.ppermute(residual, "sp", across)
    meta = jnp.concatenate([expert_ids.astype(F32), expert_weights], 1)
    far_meta = lax.ppermute(meta, "sp", across)
    other_weight = lax.ppermute(out_weight, "tp", swap)
    first_expert = (place // half * half).astype(F32)
    top = expert_ids.shape[1]
    ids, far_ids = meta[:, :top] - first_expert, far_meta[:, :top] - first_expert
    far_weights = far_meta[:, top:]

    lane = np.arange(LANES) % size
    freq = 10000.0 ** (-(lane % (size // 2)) / (size // 2))
    sign = np.where(lane < size // 2, -1.0, 1.0)
    turns = np.arange(tok_dev)[:, None] * freq
    starts = (np.arange(count) * tok_dev)[:, None] * freq
    cos_t, sin_t = jnp.asarray(np.cos(turns), F32), jnp.asarray(np.sin(turns) * sign, F32)
    bases = jnp.asarray(np.stack([np.cos(starts), np.sin(starts) * sign], 1), F32)
    base = lax.dynamic_index_in_dim(bases, place, 0, False)
    (packed,) = call(
        state_kernel,
        [((pairs * size + 16, LANES), BF16)],
        (key_vectors, value_vectors, log_decay, base, cos_t, sin_t),
        "state",
        size=size,
    )
    within, scaled = call(
        within_kernel,
        [((tok_dev, channels), F32), ((tok_dev, channels), BF16)],
        (queries, key_vectors, value_vectors, log_decay, base, cos_t, sin_t),
        "within",
        size=size,
    )
    incoming = prefix_states(packed, pairs, size)
    (normed,) = call(
        normed_kernel,
        [((tok_dev, channels), BF16)],
        (within, scaled, incoming, head_gain[None, :], gate_inputs),
        "normed",
        size=size,
    )

    axes = ("sp", "tp")
    index = [(j, c) for j in range(count) for c in range(cores)]
    mine = lax.dynamic_slice_in_dim(normed, core * tokens, tokens, 0)
    theirs = lax.dynamic_slice_in_dim(normed, (cores - 1 - core) * tokens, tokens, 0)
    flip = [(j * cores + c, j * cores + cores - 1 - c) for j, c in index]
    same = [(j * cores + c, (j + half) % count * cores + c) for j, c in index]
    cross = [(j * cores + c, (j + half) % count * cores + cores - 1 - c) for j, c in index]
    near = lax.ppermute(theirs, axes, flip)
    far_a = lax.ppermute(mine, axes, same)
    far_b = lax.ppermute(theirs, axes, cross)

    def dispatch(a, b, res, who, name):
        mixed, out = call(
            dispatch_kernel,
            [((tokens, width), BF16), ((half * capacity, width), BF16)],
            (a, b, out_weight, other_weight, res, norm_gain[None, :], who),
            name,
            capacity=capacity,
        )
        return mixed, out.reshape(half, capacity, width)

    def exchange(x):
        return lax.all_to_all(
            x, "sp", split_axis=0, concat_axis=0, tiled=True, axis_index_groups=groups
        )

    def run(received, name):
        rows = received.reshape(half * capacity, width)
        oth = lax.ppermute(rows, "tp", swap)
        p_own, p_oth = experts_call(rows, oth, gate_experts, up_experts, down_experts, name)
        back = lax.ppermute(p_oth, "tp", swap)
        total = (p_own.astype(F32) + back.astype(F32)).astype(BF16)
        return total.reshape(half, capacity, width)

    mixed, out_near = dispatch(mine, near, residual, ids, "dispatch_near")
    _, out_far = dispatch(far_a, far_b, far_res, far_ids, "dispatch_far")
    got_near = exchange(out_near)
    got_far = exchange(out_far)
    ret_near = exchange(run(got_near, "experts_near")).reshape(half * capacity, width)
    ret_far = exchange(run(got_far, "experts_far")).reshape(half * capacity, width)
    (far_sum,) = call(
        back_kernel,
        [((tokens, width), BF16)],
        (ret_far, far_ids, far_weights),
        "back_far",
        capacity=capacity,
    )
    arrived = lax.ppermute(far_sum, "sp", across)
    (part,) = call(
        own_kernel,
        [((tokens, width), F32)],
        (ret_near, ids, expert_weights),
        "back_near",
        capacity=capacity,
    )
    (out,) = call(final_kernel, [((tokens, width), BF16)], (mixed, part, arrived), "final")
    return out


def solution(mesh):
    return jax.shard_map(
        shards,
        mesh=mesh,
        in_specs=(
            P("sp", "tp"),
            P("sp", "tp"),
            P("sp", "tp"),
            P("sp", "tp"),
            P("sp", "tp"),
            P("tp"),
            P("tp", None),
            P(("sp", "tp"), None),
            P(),
            P(("sp", "tp"), None),
            P(("sp", "tp"), None),
            P("sp", None, "tp"),
            P("sp", None, "tp"),
            P("sp", "tp", None),
        ),
        out_specs=P(("sp", "tp"), None),
        check_vma=False,
    )
```

```python
import functools

import jax
import jax.numpy as jnp
import numpy as np
from jax import lax
from jax.experimental import pallas as pl
from jax.experimental.pallas import tpu as pltpu
from jax.sharding import PartitionSpec as P


BF16 = jnp.bfloat16
F32 = jnp.float32
LANES = 128
NEG = -1e30


def dot(a, b, dims=((1,), (0,)), precision=None):
    return lax.dot_general(a, b, (dims, ((), ())), precision=precision, preferred_element_type=F32)


def params(vmem):
    return pltpu.CompilerParams(vmem_limit_bytes=vmem * 1024 * 1024)


def call(kernel, outs, args, vmem, **static):
    return pl.pallas_call(
        functools.partial(kernel, **static) if static else kernel,
        out_shape=[jax.ShapeDtypeStruct(s, d) for s, d in outs],
        compiler_params=params(vmem),
    )(*args)


def staged_call(kernel, outs, args, vmem, **static):
    count, outputs = len(args), len(outs)

    def body(*refs):
        given, results = refs[:count], refs[count : count + outputs]
        local, sems = refs[count + outputs : -1], refs[-1]
        copies = [
            pltpu.make_async_copy(src, dst, sems.at[i])
            for i, (src, dst) in enumerate(zip(given, local))
        ]
        for copy in copies:
            copy.start()
        for copy in copies:
            copy.wait()
        kernel(*local, *results, **static)

    return pl.pallas_call(
        body,
        in_specs=[pl.BlockSpec(memory_space=pltpu.HBM)] * count,
        out_shape=[jax.ShapeDtypeStruct(s, d) for s, d in outs],
        scratch_shapes=[pltpu.VMEM(a.shape, a.dtype) for a in args]
        + [pltpu.SemaphoreType.DMA((count,))],
        compiler_params=params(vmem),
    )(*[pltpu.with_memory_space_constraint(a, pltpu.HBM) for a in args])


def lane_iota(rows, lanes=LANES):
    return lax.broadcasted_iota(jnp.int32, (rows, lanes), 1)


def row_iota(rows, lanes=LANES):
    return lax.broadcasted_iota(jnp.int32, (rows, lanes), 0)


def angles(base_ref, cos_ref, sin_ref):
    place = lax.axis_index("sp")
    base = base_ref[place]
    cos_base, sin_base = base[0:1, :], base[1:2, :]
    cos_t, sin_t = cos_ref[...], sin_ref[...]
    return cos_base * cos_t - sin_base * sin_t, sin_base * cos_t + cos_base * sin_t


def turn(x, cos, sin, size):
    half = size // 2
    first = lane_iota(x.shape[0]) % size < half
    other = jnp.where(first, pltpu.roll(x, LANES - half, 1), pltpu.roll(x, half, 1))
    return x * cos + other * sin


def cumulative_of(decay):
    rows = decay.shape[1]
    lower = (row_iota(rows, rows) >= lane_iota(rows, rows)).astype(F32)
    return dot(lower, decay, ((1,), (1,)), precision=lax.Precision.HIGHEST)


def spread(table, pair, rows, size):
    each = LANES // size
    lane = lane_iota(rows)
    wide = jnp.broadcast_to(table[:, pair * each : pair * each + 1], (rows, LANES))
    for i in range(1, each):
        wide = jnp.where(lane >= i * size, table[:, pair * each + i : pair * each + i + 1], wide)
    return wide


def state_kernel(k_ref, v_ref, decay_ref, base_ref, cos_ref, sin_ref, out_ref, *, size):
    rows, channels = k_ref.shape
    pairs = channels // LANES
    each = LANES // size
    cos, sin = angles(base_ref, cos_ref, sin_ref)
    cumulative = cumulative_of(decay_ref[...])
    total = cumulative[rows - 1 : rows, :]
    end = jnp.exp(total - cumulative)
    lane = lane_iota(size)
    for pair in range(pairs):
        cols = slice(pair * LANES, (pair + 1) * LANES)
        key = turn(k_ref[:, cols].astype(F32), cos, sin, size) * size ** (-0.5)
        key = (key * spread(end, pair, rows, size)).astype(BF16)
        full = dot(key, v_ref[:, cols], ((0,), (0,)))
        packed = full[0:size]
        for i in range(1, each):
            packed = jnp.where(lane >= i * size, full[i * size : (i + 1) * size], packed)
        out_ref[pair * size : (pair + 1) * size, :] = packed.astype(BF16)
    store_totals(out_ref, [spread(total, pair, 1, size) for pair in range(pairs)], size)


def store_totals(out_ref, totals, size):
    pairs = len(totals)
    low = [h - h.astype(BF16).astype(F32) for h in totals]
    fill = [jnp.zeros((16 - 2 * pairs, LANES), F32)]
    out_ref[pairs * size : pairs * size + 16, :] = jnp.concatenate(totals + low + fill, 0).astype(
        BF16
    )


def within_kernel(
    q_ref,
    k_ref,
    v_ref,
    decay_ref,
    base_ref,
    cos_ref,
    sin_ref,
    gain_ref,
    gate_ref,
    within_ref,
    scaled_ref,
    factor_ref,
    *,
    size,
):
    rows, channels = k_ref.shape
    pairs = channels // LANES
    each = LANES // size
    cos, sin = angles(base_ref, cos_ref, sin_ref)
    decay = decay_ref[...]
    cumulative = cumulative_of(decay)
    upper = (row_iota(rows, rows) <= lane_iota(rows, rows)).astype(F32)
    across = dot(decay, upper, precision=lax.Precision.HIGHEST)
    grown = jnp.exp(cumulative)
    causal = row_iota(rows, rows) >= lane_iota(rows, rows)
    lane = lane_iota(rows)
    for pair in range(pairs):
        cols = slice(pair * LANES, (pair + 1) * LANES)
        gate = gate_ref[:, cols].astype(F32)
        factor_ref[:, cols] = gain_ref[:, cols] * (gate / (1.0 + jnp.exp(-gate)))
        key = turn(k_ref[:, cols].astype(F32), cos, sin, size) * size ** (-0.5)
        query = turn(q_ref[:, cols].astype(F32), cos, sin, size)
        scaled_ref[:, cols] = (query * spread(grown, pair, rows, size)).astype(BF16)
        query = query.astype(BF16)
        value = v_ref[:, cols]
        result = jnp.zeros((rows, LANES), F32)
        for i in range(each):
            head = pair * each + i
            mine = (lane >= i * size) & (lane < (i + 1) * size)
            scores = dot(query, jnp.where(mine, key, 0.0).astype(BF16), ((1,), (1,)))
            gap = cumulative[:, head : head + 1] - across[head : head + 1, :]
            weight = jnp.exp(jnp.where(causal, gap, NEG))
            got = dot((scores * weight).astype(BF16), value)
            result = jnp.where(mine, got, result)
        within_ref[:, cols] = result


def level_shifts(count, stride, radix, last):
    out = []
    for k in range(1, radix):
        out.append([])
        for j in range(count):
            d = (j // stride) % radix
            if not (last and d + k >= radix):
                out[-1].append((j, j + ((d + k) % radix - d) * stride))
    return out


def radices_of(count):
    out = []
    while count > 1:
        radix = next(r for r in (4, 2, 3, count) if count % r == 0)
        out.append(radix)
        count //= radix
    return out


def state_of(ref, pair, size):
    return ref[pair * size : (pair + 1) * size, :].astype(F32)


def total_of(tail, pair, pairs):
    return tail[pair : pair + 1, :] + tail[pairs + pair : pairs + pair + 1, :]


def earlier(got_refs, tails, pair, pairs, size, digit, below=False):
    state = jnp.zeros((size, LANES), F32)
    total = jnp.zeros((1, LANES), F32)
    for k, (ref, tail) in enumerate(zip(got_refs, tails), 1):
        use = jnp.where(digit < k if below else digit >= k, 1.0, 0.0)
        state = state + use * jnp.exp(total) * state_of(ref, pair, size)
        total = total + use * total_of(tail, pair, pairs)
    return state, total


def level_kernel(own_ref, before_ref, *refs, pairs, size, stride, radix):
    got_refs, (all_ref, sofar_ref) = refs[: radix - 1], refs[radix - 1 :]
    digit = (lax.axis_index("sp") // stride) % radix
    base = pairs * size
    tails = [ref[base : base + 16, :].astype(F32) for ref in got_refs]
    own_tail = own_ref[base : base + 16, :].astype(F32)
    totals = []
    for pair in range(pairs):
        state, total = earlier(got_refs, tails, pair, pairs, size, digit)
        rest, behind = earlier(got_refs, tails, pair, pairs, size, digit, below=True)
        rest = rest + jnp.exp(behind) * state_of(own_ref, pair, size)
        behind = behind + total_of(own_tail, pair, pairs)
        rest = rest + jnp.exp(behind) * state
        rows = slice(pair * size, (pair + 1) * size)
        all_ref[rows, :] = rest.astype(BF16)
        totals.append(behind + total)
        old = before_ref[base + pair : base + pair + 1, :]
        sofar_ref[rows, :] = before_ref[rows, :] + jnp.exp(old) * state
        sofar_ref[base + pair : base + pair + 1, :] = old + total
    sofar_ref[base + pairs : base + 16, :] = jnp.zeros((16 - pairs, LANES), F32)
    store_totals(all_ref, totals, size)


def normed_kernel(
    within_ref, scaled_ref, factor_ref, before_ref, *refs, size, stride, radix, core_axis
):
    got_refs, (mine_ref, theirs_ref, rows_ref) = refs[: radix - 1], refs[radix - 1 :]
    rows, channels = within_ref.shape
    pairs = channels // LANES
    each = LANES // size
    base = pairs * size
    digit = (lax.axis_index("sp") // stride) % radix
    tails = [ref[base : base + 16, :].astype(F32) for ref in got_refs]
    lane = lane_iota(rows)
    lane_s = lane_iota(size)
    for pair in range(pairs):
        cols = slice(pair * LANES, (pair + 1) * LANES)
        state, _ = earlier(got_refs, tails, pair, pairs, size, digit)
        old = before_ref[base + pair : base + pair + 1, :]
        packed = before_ref[pair * size : (pair + 1) * size, :] + jnp.exp(old) * state
        blocks = [
            jnp.where((lane_s >= i * size) & (lane_s < (i + 1) * size), packed, 0.0)
            for i in range(each)
        ]
        incoming = jnp.concatenate(blocks, 0).astype(BF16)
        retained = within_ref[:, cols] + dot(scaled_ref[:, cols], incoming)
        squares = retained * retained
        mean = jnp.zeros((rows, LANES), F32)
        for i in range(each):
            mine = (lane >= i * size) & (lane < (i + 1) * size)
            part = jnp.sum(jnp.where(mine, squares, 0.0), axis=1, keepdims=True) * (1.0 / size)
            mean = jnp.where(mine, part, mean)
        out = retained * lax.rsqrt(mean + 1e-06) * factor_ref[:, cols]
        rows_ref[:, cols] = out.astype(BF16)
    tokens = mine_ref.shape[0]
    core = lax.axis_index(core_axis)
    mine_ref[...] = rows_ref[pl.ds(pl.multiple_of(core * tokens, tokens), tokens), :]
    theirs_ref[...] = rows_ref[pl.ds(pl.multiple_of((1 - core) * tokens, tokens), tokens), :]


def meta_of(meta_ref, top):
    meta = meta_ref[...].T
    first = meta[:, 2 * top : 2 * top + 1]
    return meta[:, :top] - first, meta[:, top : 2 * top]


def slots_of(ids, capacity, slots):
    tokens = ids.shape[0]
    lane = lane_iota(tokens).astype(F32)
    named = [lane == ids[:, j : j + 1] for j in range(ids.shape[1])]
    member = functools.reduce(jnp.logical_or, named).astype(BF16)
    strict = (row_iota(tokens, tokens) > lane_iota(tokens, tokens)).astype(BF16)
    rank = dot(strict, member)
    place = lane_iota(tokens, slots).astype(F32)
    out = []
    for j, hit in enumerate(named):
        slot = ids[:, j : j + 1] * capacity + jnp.sum(jnp.where(hit, rank, 0.0), 1, keepdims=True)
        out.append(place == slot)
    return out


def dispatch_kernel(
    a_ref, b_ref, wa_ref, wb_ref, res_ref, gain_ref, meta_ref, mixed_ref, out_ref, *, capacity, top
):
    projected = dot(a_ref[...], wa_ref[...]).astype(BF16).astype(F32)
    projected = projected + dot(b_ref[...], wb_ref[...]).astype(BF16).astype(F32)
    mixed = (res_ref[...].astype(F32) + projected).astype(BF16)
    mixed_ref[...] = mixed
    wide = mixed.astype(F32)
    scale = lax.rsqrt(jnp.mean(wide * wide, axis=1, keepdims=True) + 1e-06)
    rows = (wide * scale * gain_ref[...]).astype(BF16)
    ids, _ = meta_of(meta_ref, top)
    hot = functools.reduce(jnp.logical_or, slots_of(ids, capacity, out_ref.shape[0]))
    out_ref[...] = dot(hot.astype(BF16), rows, ((0,), (0,))).astype(BF16)


def expert_kernel(
    own_ref, oth_ref, gate_ref, up_ref, down_ref, pown_ref, poth_ref, hidden_ref, *, first
):
    step = pl.program_id(0)
    count = own_ref.shape[0]
    tile = gate_ref.shape[1]

    @pl.when(step < first)
    def _():
        rows = jnp.concatenate([own_ref[...], oth_ref[...]], 0)
        gate = dot(rows, gate_ref[...])
        up = dot(rows, up_ref[...])
        hidden = (gate / (1.0 + jnp.exp(-gate)) * up).astype(BF16)
        hidden_ref[:, pl.ds(pl.multiple_of(step * tile, tile), tile)] = hidden

    @pl.when(step >= first)
    def _():
        part = dot(hidden_ref[...], down_ref[...])
        pown_ref[...] = part[:count].astype(BF16)
        poth_ref[...] = part[count:].astype(BF16)


def experts_call(own, oth, gate, up, down):
    rows, width = own.shape
    hidden = gate.shape[2]
    tile = next(t for t in (256, 128, hidden) if hidden % t == 0)
    wide = next(t for t in (512, 256, 128, width) if width % t == 0)
    first, last = hidden // tile, width // wide
    whole = pl.BlockSpec((rows, width), lambda i: (0, 0))
    part = pl.BlockSpec((rows, wide), lambda i: (0, jnp.maximum(i - first, 0)))
    entry = pl.BlockSpec((None, width, tile), lambda i: (0, 0, jnp.minimum(i, first - 1)))
    return pl.pallas_call(
        functools.partial(expert_kernel, first=first),
        grid=(first + last,),
        in_specs=[
            whole,
            whole,
            entry,
            entry,
            pl.BlockSpec((None, hidden, wide), lambda i: (0, 0, jnp.maximum(i - first, 0))),
        ],
        out_specs=[part, part],
        out_shape=[jax.ShapeDtypeStruct((rows, width), BF16)] * 2,
        scratch_shapes=[pltpu.VMEM((2 * rows, hidden), BF16)],
        compiler_params=params(32),
        cost_estimate=pl.CostEstimate(
            flops=2 * rows * 6 * width * hidden,
            bytes_accessed=6 * width * hidden,
            transcendentals=2 * rows * hidden,
        ),
    )(own, oth, *[pltpu.with_memory_space_constraint(w, pltpu.HBM) for w in (gate, up, down)])


def gather_sum(ret, ids, weights, capacity):
    hots = slots_of(ids, capacity, ret.shape[0])
    total = None
    for j, hot in enumerate(hots):
        part = dot(hot.astype(BF16), ret) * weights[:, j : j + 1]
        total = part if total is None else total + part
    return total


def back_kernel(ret_ref, meta_ref, out_ref, *, capacity, top):
    ids, weights = meta_of(meta_ref, top)
    out_ref[...] = gather_sum(ret_ref[...], ids, weights, capacity).astype(out_ref.dtype)


def final_kernel(mixed_ref, part_ref, far_ref, out_ref):
    total = part_ref[...] + far_ref[...].astype(F32)
    out_ref[...] = (mixed_ref[...].astype(F32) + total).astype(BF16)


def shards(
    queries,
    key_vectors,
    value_vectors,
    gate_inputs,
    log_decay,
    head_gain,
    out_weight,
    residual,
    norm_gain,
    expert_ids,
    expert_weights,
    gate_experts,
    up_experts,
    down_experts,
):
    tok_dev, channels = queries.shape
    heads = log_decay.shape[1]
    size = channels // heads
    pairs = channels // LANES
    tokens, width = residual.shape
    count = lax.axis_size("sp")
    cores = lax.axis_size("tp")
    half = count // 2
    capacity = 2 * tok_dev // count
    place = lax.axis_index("sp")
    across = [(j, (j + half) % count) for j in range(count)]
    swap = [(c, cores - 1 - c) for c in range(cores)]
    groups = [list(range(half)), list(range(half, count))]

    top = expert_ids.shape[1]

    def meta_for(where):
        first = jnp.broadcast_to((where // half * half).astype(F32), (1, tokens))
        fill = jnp.zeros((8 - 2 * top - 1, tokens), F32)
        return jnp.concatenate([expert_ids.T.astype(F32), expert_weights.T, first, fill], 0)

    far_res = lax.ppermute(residual, "sp", across)
    other_weight = lax.ppermute(out_weight, "tp", swap)
    meta = meta_for(place)
    far_meta = lax.ppermute(meta_for((place + half) % count), "sp", across)

    lane = np.arange(LANES) % size
    freq = 10000.0 ** (-(lane % (size // 2)) / (size // 2))
    sign = np.where(lane < size // 2, -1.0, 1.0)
    turns = np.arange(tok_dev)[:, None] * freq
    starts = (np.arange(count) * tok_dev)[:, None] * freq
    cos_t, sin_t = jnp.asarray(np.cos(turns), F32), jnp.asarray(np.sin(turns) * sign, F32)
    bases = np.zeros((count, 8, LANES), np.float32)
    bases[:, 0], bases[:, 1] = np.cos(starts), np.sin(starts) * sign
    bases = jnp.asarray(bases)
    decay = log_decay.T
    (own,) = staged_call(
        state_kernel,
        [((pairs * size + 16, LANES), BF16)],
        (key_vectors, value_vectors, decay, bases, cos_t, sin_t),
        12,
        size=size,
    )
    within, scaled, factor = staged_call(
        within_kernel,
        [((tok_dev, channels), F32), ((tok_dev, channels), BF16), ((tok_dev, channels), F32)],
        (
            queries,
            key_vectors,
            value_vectors,
            decay,
            bases,
            cos_t,
            sin_t,
            head_gain[None, :],
            gate_inputs,
        ),
        20,
        size=size,
    )
    levels = radices_of(count)
    before = jnp.zeros((pairs * size + 16, LANES), F32)
    stride = 1
    for level, radix in enumerate(levels):
        last = level == len(levels) - 1
        got = [lax.ppermute(own, "sp", p) for p in level_shifts(count, stride, radix, last)]
        if not last:
            own, before = call(
                level_kernel,
                [(own.shape, BF16), (before.shape, F32)],
                (own, before, *got),
                8,
                pairs=pairs,
                size=size,
                stride=stride,
                radix=radix,
            )
            stride *= radix
    mine, theirs = pl.pallas_call(
        functools.partial(normed_kernel, size=size, stride=stride, radix=radix, core_axis="tp"),
        out_shape=[jax.ShapeDtypeStruct((tokens, channels), BF16)] * 2,
        scratch_shapes=[pltpu.VMEM((tok_dev, channels), BF16)],
        compiler_params=params(12),
        name="normed",
    )(within, scaled, factor, before, *got)

    axes = ("sp", "tp")
    index = [(j, c) for j in range(count) for c in range(cores)]
    flip = [(j * cores + c, j * cores + cores - 1 - c) for j, c in index]
    same = [(j * cores + c, (j + half) % count * cores + c) for j, c in index]
    cross = [(j * cores + c, (j + half) % count * cores + cores - 1 - c) for j, c in index]
    near = lax.ppermute(theirs, axes, flip)
    far_a = lax.ppermute(mine, axes, same)
    far_b = lax.ppermute(theirs, axes, cross)

    def dispatch(a, b, res, who):
        mixed, out = call(
            dispatch_kernel,
            [((tokens, width), BF16), ((half * capacity, width), BF16)],
            (a, b, out_weight, other_weight, res, norm_gain[None, :], who),
            20,
            capacity=capacity,
            top=top,
        )
        return mixed, out.reshape(half, capacity, width)

    def exchange(x):
        return lax.all_to_all(
            x, "sp", split_axis=0, concat_axis=0, tiled=True, axis_index_groups=groups
        )

    def run(received):
        rows = received.reshape(half * capacity, width)
        oth = lax.ppermute(rows, "tp", swap)
        p_own, p_oth = experts_call(rows, oth, gate_experts, up_experts, down_experts)
        back = lax.ppermute(p_oth, "tp", swap)
        total = (p_own.astype(F32) + back.astype(F32)).astype(BF16)
        return total.reshape(half, capacity, width)

    def back(returned, who, dtype):
        (out,) = call(
            back_kernel,
            [((tokens, width), dtype)],
            (returned.reshape(half * capacity, width), who),
            16,
            capacity=capacity,
            top=top,
        )
        return out

    mixed, out_near = dispatch(mine, near, residual, meta)
    got_near = exchange(out_near)
    _, out_far = dispatch(far_a, far_b, far_res, far_meta)
    got_far = exchange(out_far)
    ret_near = exchange(run(got_near))
    ret_far = exchange(run(got_far))
    part = back(ret_near, meta, F32)
    far_sum = back(ret_far, far_meta, BF16)
    arrived = lax.ppermute(far_sum, "sp", across)
    (out,) = call(final_kernel, [((tokens, width), BF16)], (mixed, part, arrived), 12)
    return out


def solution(mesh):
    return jax.shard_map(
        shards,
        mesh=mesh,
        in_specs=(
            P("sp", "tp"),
            P("sp", "tp"),
            P("sp", "tp"),
            P("sp", "tp"),
            P("sp", "tp"),
            P("tp"),
            P("tp", None),
            P(("sp", "tp"), None),
            P(),
            P(("sp", "tp"), None),
            P(("sp", "tp"), None),
            P("sp", None, "tp"),
            P("sp", None, "tp"),
            P("sp", "tp", None),
        ),
        out_specs=P(("sp", "tp"), None),
        check_vma=False,
    )
```

```python
import functools

import jax
import jax.numpy as jnp
import numpy as np
from jax import lax
from jax.experimental import pallas as pl
from jax.experimental.pallas import tpu as pltpu
from jax.sharding import PartitionSpec as P


BF16 = jnp.bfloat16
F32 = jnp.float32
LANES = 128
NEG = -1e30


def dot(a, b, dims=((1,), (0,)), precision=None):
    return lax.dot_general(a, b, (dims, ((), ())), precision=precision, preferred_element_type=F32)


def params(vmem):
    return pltpu.CompilerParams(vmem_limit_bytes=vmem * 1024 * 1024)


def call(kernel, outs, args, vmem, **static):
    return pl.pallas_call(
        functools.partial(kernel, **static) if static else kernel,
        out_shape=[jax.ShapeDtypeStruct(s, d) for s, d in outs],
        compiler_params=params(vmem),
    )(*args)


def staged_call(kernel, outs, args, vmem, **static):
    count, outputs = len(args), len(outs)

    def body(*refs):
        given, results = refs[:count], refs[count : count + outputs]
        local, sems = refs[count + outputs : -1], refs[-1]
        copies = [
            pltpu.make_async_copy(src, dst, sems.at[i])
            for i, (src, dst) in enumerate(zip(given, local))
        ]
        for copy in copies:
            copy.start()
        for copy in copies:
            copy.wait()
        kernel(*local, *results, **static)

    return pl.pallas_call(
        body,
        in_specs=[pl.BlockSpec(memory_space=pltpu.HBM)] * count,
        out_shape=[jax.ShapeDtypeStruct(s, d) for s, d in outs],
        scratch_shapes=[pltpu.VMEM(a.shape, a.dtype) for a in args]
        + [pltpu.SemaphoreType.DMA((count,))],
        compiler_params=params(vmem),
    )(*[pltpu.with_memory_space_constraint(a, pltpu.HBM) for a in args])


def lane_iota(rows, lanes=LANES):
    return lax.broadcasted_iota(jnp.int32, (rows, lanes), 1)


def row_iota(rows, lanes=LANES):
    return lax.broadcasted_iota(jnp.int32, (rows, lanes), 0)


def angles(base_ref, cos_ref, sin_ref):
    place = lax.axis_index("sp")
    base = base_ref[place]
    cos_base, sin_base = base[0:1, :], base[1:2, :]
    cos_t, sin_t = cos_ref[...], sin_ref[...]
    return cos_base * cos_t - sin_base * sin_t, sin_base * cos_t + cos_base * sin_t


def turn(x, cos, sin, size):
    half = size // 2
    first = lane_iota(x.shape[0]) % size < half
    other = jnp.where(first, pltpu.roll(x, LANES - half, 1), pltpu.roll(x, half, 1))
    return x * cos + other * sin


def cumulative_of(decay):
    rows = decay.shape[1]
    lower = (row_iota(rows, rows) >= lane_iota(rows, rows)).astype(F32)
    return dot(lower, decay, ((1,), (1,)), precision=lax.Precision.HIGHEST)


def spread(table, pair, rows, size):
    each = LANES // size
    lane = lane_iota(rows)
    wide = jnp.broadcast_to(table[:, pair * each : pair * each + 1], (rows, LANES))
    for i in range(1, each):
        wide = jnp.where(lane >= i * size, table[:, pair * each + i : pair * each + i + 1], wide)
    return wide


def state_kernel(k_ref, v_ref, decay_ref, base_ref, cos_ref, sin_ref, out_ref, *, size):
    rows, channels = k_ref.shape
    pairs = channels // LANES
    each = LANES // size
    cos, sin = angles(base_ref, cos_ref, sin_ref)
    cumulative = cumulative_of(decay_ref[...])
    total = cumulative[rows - 1 : rows, :]
    end = jnp.exp(total - cumulative)
    lane = lane_iota(size)
    for pair in range(pairs):
        cols = slice(pair * LANES, (pair + 1) * LANES)
        key = turn(k_ref[:, cols].astype(F32), cos, sin, size) * size ** (-0.5)
        key = (key * spread(end, pair, rows, size)).astype(BF16)
        full = dot(key, v_ref[:, cols], ((0,), (0,)))
        packed = full[0:size]
        for i in range(1, each):
            packed = jnp.where(lane >= i * size, full[i * size : (i + 1) * size], packed)
        out_ref[pair * size : (pair + 1) * size, :] = packed.astype(BF16)
    store_totals(out_ref, [spread(total, pair, 1, size) for pair in range(pairs)], size)


def store_totals(out_ref, totals, size):
    pairs = len(totals)
    low = [h - h.astype(BF16).astype(F32) for h in totals]
    fill = [jnp.zeros((16 - 2 * pairs, LANES), F32)]
    out_ref[pairs * size : pairs * size + 16, :] = jnp.concatenate(totals + low + fill, 0).astype(
        BF16
    )


def within_kernel(
    q_ref,
    k_ref,
    v_ref,
    decay_ref,
    base_ref,
    cos_ref,
    sin_ref,
    gain_ref,
    gate_ref,
    within_ref,
    scaled_ref,
    factor_ref,
    *,
    size,
):
    rows, channels = k_ref.shape
    pairs = channels // LANES
    each = LANES // size
    cos, sin = angles(base_ref, cos_ref, sin_ref)
    decay = decay_ref[...]
    cumulative = cumulative_of(decay)
    upper = (row_iota(rows, rows) <= lane_iota(rows, rows)).astype(F32)
    across = dot(decay, upper, precision=lax.Precision.HIGHEST)
    grown = jnp.exp(cumulative)
    causal = row_iota(rows, rows) >= lane_iota(rows, rows)
    lane = lane_iota(rows)
    for pair in range(pairs):
        cols = slice(pair * LANES, (pair + 1) * LANES)
        gate = gate_ref[:, cols].astype(F32)
        factor_ref[:, cols] = gain_ref[:, cols] * (gate / (1.0 + jnp.exp(-gate)))
        key = turn(k_ref[:, cols].astype(F32), cos, sin, size) * size ** (-0.5)
        query = turn(q_ref[:, cols].astype(F32), cos, sin, size)
        scaled_ref[:, cols] = (query * spread(grown, pair, rows, size)).astype(BF16)
        query = query.astype(BF16)
        value = v_ref[:, cols]
        result = jnp.zeros((rows, LANES), F32)
        for i in range(each):
            head = pair * each + i
            mine = (lane >= i * size) & (lane < (i + 1) * size)
            scores = dot(query, jnp.where(mine, key, 0.0).astype(BF16), ((1,), (1,)))
            gap = cumulative[:, head : head + 1] - across[head : head + 1, :]
            weight = jnp.exp(jnp.where(causal, gap, NEG))
            got = dot((scores * weight).astype(BF16), value)
            result = jnp.where(mine, got, result)
        within_ref[:, cols] = result


def level_shifts(count, stride, radix, last):
    out = []
    for k in range(1, radix):
        out.append([])
        for j in range(count):
            d = (j // stride) % radix
            if not (last and d + k >= radix):
                out[-1].append((j, j + ((d + k) % radix - d) * stride))
    return out


def radices_of(count):
    out = []
    while count > 1:
        radix = next(r for r in (4, 2, 3, count) if count % r == 0)
        out.append(radix)
        count //= radix
    return out


def state_of(ref, pair, size):
    return ref[pair * size : (pair + 1) * size, :].astype(F32)


def total_of(tail, pair, pairs):
    return tail[pair : pair + 1, :] + tail[pairs + pair : pairs + pair + 1, :]


def earlier(got_refs, tails, pair, pairs, size, digit, below=False):
    state = jnp.zeros((size, LANES), F32)
    total = jnp.zeros((1, LANES), F32)
    for k, (ref, tail) in enumerate(zip(got_refs, tails), 1):
        use = jnp.where(digit < k if below else digit >= k, 1.0, 0.0)
        state = state + use * jnp.exp(total) * state_of(ref, pair, size)
        total = total + use * total_of(tail, pair, pairs)
    return state, total


def level_kernel(own_ref, before_ref, *refs, pairs, size, stride, radix):
    got_refs, (all_ref, sofar_ref) = refs[: radix - 1], refs[radix - 1 :]
    digit = (lax.axis_index("sp") // stride) % radix
    base = pairs * size
    tails = [ref[base : base + 16, :].astype(F32) for ref in got_refs]
    own_tail = own_ref[base : base + 16, :].astype(F32)
    totals = []
    for pair in range(pairs):
        state, total = earlier(got_refs, tails, pair, pairs, size, digit)
        rest, behind = earlier(got_refs, tails, pair, pairs, size, digit, below=True)
        rest = rest + jnp.exp(behind) * state_of(own_ref, pair, size)
        behind = behind + total_of(own_tail, pair, pairs)
        rest = rest + jnp.exp(behind) * state
        rows = slice(pair * size, (pair + 1) * size)
        all_ref[rows, :] = rest.astype(BF16)
        totals.append(behind + total)
        old = before_ref[base + pair : base + pair + 1, :]
        sofar_ref[rows, :] = before_ref[rows, :] + jnp.exp(old) * state
        sofar_ref[base + pair : base + pair + 1, :] = old + total
    sofar_ref[base + pairs : base + 16, :] = jnp.zeros((16 - pairs, LANES), F32)
    store_totals(all_ref, totals, size)


def normed_kernel(
    within_ref, scaled_ref, factor_ref, before_ref, *refs, size, stride, radix, core_axis
):
    got_refs, (mine_ref, theirs_ref, rows_ref) = refs[: radix - 1], refs[radix - 1 :]
    rows, channels = within_ref.shape
    pairs = channels // LANES
    each = LANES // size
    base = pairs * size
    digit = (lax.axis_index("sp") // stride) % radix
    tails = [ref[base : base + 16, :].astype(F32) for ref in got_refs]
    lane = lane_iota(rows)
    lane_s = lane_iota(size)
    for pair in range(pairs):
        cols = slice(pair * LANES, (pair + 1) * LANES)
        state, _ = earlier(got_refs, tails, pair, pairs, size, digit)
        old = before_ref[base + pair : base + pair + 1, :]
        packed = before_ref[pair * size : (pair + 1) * size, :] + jnp.exp(old) * state
        blocks = [
            jnp.where((lane_s >= i * size) & (lane_s < (i + 1) * size), packed, 0.0)
            for i in range(each)
        ]
        incoming = jnp.concatenate(blocks, 0).astype(BF16)
        retained = within_ref[:, cols] + dot(scaled_ref[:, cols], incoming)
        squares = retained * retained
        mean = jnp.zeros((rows, LANES), F32)
        for i in range(each):
            mine = (lane >= i * size) & (lane < (i + 1) * size)
            part = jnp.sum(jnp.where(mine, squares, 0.0), axis=1, keepdims=True) * (1.0 / size)
            mean = jnp.where(mine, part, mean)
        out = retained * lax.rsqrt(mean + 1e-06) * factor_ref[:, cols]
        rows_ref[:, cols] = out.astype(BF16)
    tokens = mine_ref.shape[0]
    core = lax.axis_index(core_axis)
    mine_ref[...] = rows_ref[pl.ds(pl.multiple_of(core * tokens, tokens), tokens), :]
    theirs_ref[...] = rows_ref[pl.ds(pl.multiple_of((1 - core) * tokens, tokens), tokens), :]


def meta_of(meta_ref, top):
    meta = meta_ref[...].T
    first = meta[:, 2 * top : 2 * top + 1]
    return meta[:, :top] - first, meta[:, top : 2 * top]


def slots_of(ids, capacity, slots):
    tokens = ids.shape[0]
    lane = lane_iota(tokens).astype(F32)
    named = [lane == ids[:, j : j + 1] for j in range(ids.shape[1])]
    member = functools.reduce(jnp.logical_or, named).astype(BF16)
    strict = (row_iota(tokens, tokens) > lane_iota(tokens, tokens)).astype(BF16)
    rank = dot(strict, member)
    place = lane_iota(tokens, slots).astype(F32)
    out = []
    for j, hit in enumerate(named):
        slot = ids[:, j : j + 1] * capacity + jnp.sum(jnp.where(hit, rank, 0.0), 1, keepdims=True)
        out.append(place == slot)
    return out


def dispatch_kernel(
    a_ref, b_ref, wa_ref, wb_ref, res_ref, gain_ref, meta_ref, mixed_ref, out_ref, *, capacity, top
):
    projected = dot(a_ref[...], wa_ref[...]).astype(BF16).astype(F32)
    projected = projected + dot(b_ref[...], wb_ref[...]).astype(BF16).astype(F32)
    mixed = (res_ref[...].astype(F32) + projected).astype(BF16)
    mixed_ref[...] = mixed
    wide = mixed.astype(F32)
    scale = lax.rsqrt(jnp.mean(wide * wide, axis=1, keepdims=True) + 1e-06)
    rows = (wide * scale * gain_ref[...]).astype(BF16)
    ids, _ = meta_of(meta_ref, top)
    hot = functools.reduce(jnp.logical_or, slots_of(ids, capacity, out_ref.shape[0]))
    out_ref[...] = dot(hot.astype(BF16), rows, ((0,), (0,))).astype(BF16)


def expert_kernel(
    own_ref, oth_ref, gate_ref, up_ref, down_ref, pown_ref, poth_ref, hidden_ref, *, first
):
    step = pl.program_id(0)
    count = own_ref.shape[0]
    tile = gate_ref.shape[1]

    @pl.when(step < first)
    def _():
        rows = jnp.concatenate([own_ref[...], oth_ref[...]], 0)
        gate = dot(rows, gate_ref[...])
        up = dot(rows, up_ref[...])
        hidden = (gate / (1.0 + jnp.exp(-gate)) * up).astype(BF16)
        hidden_ref[:, pl.ds(pl.multiple_of(step * tile, tile), tile)] = hidden

    @pl.when(step >= first)
    def _():
        part = dot(hidden_ref[...], down_ref[...])
        pown_ref[...] = part[:count].astype(BF16)
        poth_ref[...] = part[count:].astype(BF16)


def experts_call(own, oth, gate, up, down):
    rows, width = own.shape
    hidden = gate.shape[2]
    tile = next(t for t in (256, 128, hidden) if hidden % t == 0)
    wide = next(t for t in (1024, 512, 256, 128, width) if width % t == 0)
    first, last = hidden // tile, width // wide
    whole = pl.BlockSpec((rows, width), lambda i: (0, 0))
    part = pl.BlockSpec((rows, wide), lambda i: (0, jnp.maximum(i - first, 0)))
    entry = pl.BlockSpec((None, width, tile), lambda i: (0, 0, jnp.minimum(i, first - 1)))
    return pl.pallas_call(
        functools.partial(expert_kernel, first=first),
        grid=(first + last,),
        in_specs=[
            whole,
            whole,
            entry,
            entry,
            pl.BlockSpec((None, hidden, wide), lambda i: (0, 0, jnp.maximum(i - first, 0))),
        ],
        out_specs=[part, part],
        out_shape=[jax.ShapeDtypeStruct((rows, width), BF16)] * 2,
        scratch_shapes=[pltpu.VMEM((2 * rows, hidden), BF16)],
        compiler_params=params(24),
        cost_estimate=pl.CostEstimate(
            flops=2 * rows * 6 * width * hidden,
            bytes_accessed=6 * width * hidden,
            transcendentals=2 * rows * hidden,
        ),
    )(own, oth, *[pltpu.with_memory_space_constraint(w, pltpu.HBM) for w in (gate, up, down)])


def gather_sum(ret, ids, weights, capacity):
    hots = slots_of(ids, capacity, ret.shape[0])
    total = None
    for j, hot in enumerate(hots):
        part = dot(hot.astype(BF16), ret) * weights[:, j : j + 1]
        total = part if total is None else total + part
    return total


def back_kernel(ret_ref, meta_ref, out_ref, *, capacity, top):
    ids, weights = meta_of(meta_ref, top)
    out_ref[...] = gather_sum(ret_ref[...], ids, weights, capacity).astype(out_ref.dtype)


def join_kernel(own_ref, back_ref, out_ref):
    out_ref[...] = (own_ref[...].astype(F32) + back_ref[...].astype(F32)).astype(BF16)


def final_kernel(mixed_ref, part_ref, far_ref, out_ref):
    total = part_ref[...] + far_ref[...].astype(F32)
    out_ref[...] = (mixed_ref[...].astype(F32) + total).astype(BF16)


def shards(
    queries,
    key_vectors,
    value_vectors,
    gate_inputs,
    log_decay,
    head_gain,
    out_weight,
    residual,
    norm_gain,
    expert_ids,
    expert_weights,
    gate_experts,
    up_experts,
    down_experts,
):
    tok_dev, channels = queries.shape
    heads = log_decay.shape[1]
    size = channels // heads
    pairs = channels // LANES
    tokens, width = residual.shape
    count = lax.axis_size("sp")
    cores = lax.axis_size("tp")
    half = count // 2
    capacity = 2 * tok_dev // count
    place = lax.axis_index("sp")
    across = [(j, (j + half) % count) for j in range(count)]
    swap = [(c, cores - 1 - c) for c in range(cores)]
    groups = [list(range(half)), list(range(half, count))]

    top = expert_ids.shape[1]

    def meta_for(where):
        first = jnp.broadcast_to((where // half * half).astype(F32), (1, tokens))
        fill = jnp.zeros((8 - 2 * top - 1, tokens), F32)
        return jnp.concatenate([expert_ids.T.astype(F32), expert_weights.T, first, fill], 0)

    far_res = lax.ppermute(residual, "sp", across)
    other_weight = lax.ppermute(out_weight, "tp", swap)
    meta = meta_for(place)
    far_meta = lax.ppermute(meta_for((place + half) % count), "sp", across)

    lane = np.arange(LANES) % size
    freq = 10000.0 ** (-(lane % (size // 2)) / (size // 2))
    sign = np.where(lane < size // 2, -1.0, 1.0)
    turns = np.arange(tok_dev)[:, None] * freq
    starts = (np.arange(count) * tok_dev)[:, None] * freq
    cos_t, sin_t = jnp.asarray(np.cos(turns), F32), jnp.asarray(np.sin(turns) * sign, F32)
    bases = np.zeros((count, 8, LANES), np.float32)
    bases[:, 0], bases[:, 1] = np.cos(starts), np.sin(starts) * sign
    bases = jnp.asarray(bases)
    decay = log_decay.T
    (own,) = staged_call(
        state_kernel,
        [((pairs * size + 16, LANES), BF16)],
        (key_vectors, value_vectors, decay, bases, cos_t, sin_t),
        12,
        size=size,
    )
    within, scaled, factor = staged_call(
        within_kernel,
        [((tok_dev, channels), F32), ((tok_dev, channels), BF16), ((tok_dev, channels), F32)],
        (
            queries,
            key_vectors,
            value_vectors,
            decay,
            bases,
            cos_t,
            sin_t,
            head_gain[None, :],
            gate_inputs,
        ),
        20,
        size=size,
    )
    levels = radices_of(count)
    before = jnp.zeros((pairs * size + 16, LANES), F32)
    stride = 1
    for level, radix in enumerate(levels):
        last = level == len(levels) - 1
        got = [lax.ppermute(own, "sp", p) for p in level_shifts(count, stride, radix, last)]
        if not last:
            own, before = call(
                level_kernel,
                [(own.shape, BF16), (before.shape, F32)],
                (own, before, *got),
                8,
                pairs=pairs,
                size=size,
                stride=stride,
                radix=radix,
            )
            stride *= radix
    mine, theirs = pl.pallas_call(
        functools.partial(normed_kernel, size=size, stride=stride, radix=radix, core_axis="tp"),
        out_shape=[jax.ShapeDtypeStruct((tokens, channels), BF16)] * 2,
        scratch_shapes=[pltpu.VMEM((tok_dev, channels), BF16)],
        compiler_params=params(12),
        name="normed",
    )(within, scaled, factor, before, *got)

    axes = ("sp", "tp")
    index = [(j, c) for j in range(count) for c in range(cores)]
    flip = [(j * cores + c, j * cores + cores - 1 - c) for j, c in index]
    same = [(j * cores + c, (j + half) % count * cores + c) for j, c in index]
    cross = [(j * cores + c, (j + half) % count * cores + cores - 1 - c) for j, c in index]
    near = lax.ppermute(theirs, axes, flip)
    far_a = lax.ppermute(mine, axes, same)
    far_b = lax.ppermute(theirs, axes, cross)

    def dispatch(a, b, res, who):
        mixed, out = call(
            dispatch_kernel,
            [((tokens, width), BF16), ((half * capacity, width), BF16)],
            (a, b, out_weight, other_weight, res, norm_gain[None, :], who),
            20,
            capacity=capacity,
            top=top,
        )
        return mixed, out.reshape(half, capacity, width)

    def exchange(x):
        return lax.all_to_all(
            x, "sp", split_axis=0, concat_axis=0, tiled=True, axis_index_groups=groups
        )

    def run(received):
        rows = received.reshape(half * capacity, width)
        oth = lax.ppermute(rows, "tp", swap)
        p_own, p_oth = experts_call(rows, oth, gate_experts, up_experts, down_experts)
        back = lax.ppermute(p_oth, "tp", swap)
        (total,) = call(join_kernel, [(rows.shape, BF16)], (p_own, back), 12)
        return total.reshape(half, capacity, width)

    def back(returned, who, dtype):
        (out,) = call(
            back_kernel,
            [((tokens, width), dtype)],
            (returned.reshape(half * capacity, width), who),
            16,
            capacity=capacity,
            top=top,
        )
        return out

    mixed, out_near = dispatch(mine, near, residual, meta)
    got_near = exchange(out_near)
    _, out_far = dispatch(far_a, far_b, far_res, far_meta)
    got_far = exchange(out_far)
    ret_near = exchange(run(got_near))
    ret_far = exchange(run(got_far))
    part = back(ret_near, meta, F32)
    far_sum = back(ret_far, far_meta, BF16)
    arrived = lax.ppermute(far_sum, "sp", across)
    (out,) = call(final_kernel, [((tokens, width), BF16)], (mixed, part, arrived), 12)
    return out


def solution(mesh):
    return jax.shard_map(
        shards,
        mesh=mesh,
        in_specs=(
            P("sp", "tp"),
            P("sp", "tp"),
            P("sp", "tp"),
            P("sp", "tp"),
            P("sp", "tp"),
            P("tp"),
            P("tp", None),
            P(("sp", "tp"), None),
            P(),
            P(("sp", "tp"), None),
            P(("sp", "tp"), None),
            P("sp", None, "tp"),
            P("sp", None, "tp"),
            P("sp", "tp", None),
        ),
        out_specs=P(("sp", "tp"), None),
        check_vma=False,
    )
```
